32 devices in a mesh: ep: 8 (over z, core), tp: 4 (over y, x).
Axes of the slice: x: 2, y: 2, z: 4, core: 2. Of those that a mesh axis runs over, the one named last changes fastest.
Arguments:
- mix_input: bfloat16 [1024, 2048], P('ep'), may hold values from -8 to 8
- expert_input: bfloat16 [1024, 2048], P('ep'), may hold values from -8 to 8
- mix_gain: float32 [2048], replicated, may hold values from 0.1 to 1.9
- moe_gain: float32 [2048], replicated, may hold values from 0.1 to 1.9
- pool_in: bfloat16 [2048, 1024], P(None, 'tp'), may hold values from -0.125 to 0.125
- pool_scale: float32 [1024], P('tp'), may hold values from 0.25 to 10
- pool_gain: float32 [1024], P('tp'), may hold values from 0.1 to 1.9
- pool_out: bfloat16 [1024, 2048], P(None, 'tp'), may hold values from -0.1875 to 0.1875
- route: int32 [1024, 4], P('ep'), may hold values from 0 to 7, all different within a row; in each aligned block of 128 rows (0 to 127, 128 to 255, ...) at most 128 rows name the same one
- route_score: float32 [1024, 4], P('ep'), may hold values from 0.05 to 1
- expert_gate: bfloat16 [8, 2048, 2048], P('ep', None, 'tp'), may hold values from -0.125 to 0.125
- expert_up: bfloat16 [8, 2048, 2048], P('ep', None, 'tp'), may hold values from -0.125 to 0.125
- expert_down: bfloat16 [8, 2048, 2048], P('ep', 'tp'), may hold values from -0.1875 to 0.1875
- shared_gate: bfloat16 [2048, 2048], P(None, 'tp'), may hold values from -0.125 to 0.125
- shared_up: bfloat16 [2048, 2048], P(None, 'tp'), may hold values from -0.125 to 0.125
- shared_down: bfloat16 [2048, 2048], P(None, 'tp'), may hold values from -0.125 to 0.125
Outputs:
- mix_out: bfloat16 [1024, 2048], P('ep', 'tp')
- moe_out: bfloat16 [1024, 2048], P('ep', 'tp')
The draws below stay inside these ranges and needn't reach their ends.
Inputs may be any that keep to these rules, and one draw needn't show every extreme that they name: `route`: each row names 4 different experts. In the rows of one index of ep (aligned blocks of 128 rows) no expert is named more than 128 times, a bound that some block reaches.
All inputs are finite; a program needn't handle non-finite values.
Results may differ from the reference program's by a relative error of at most 0.014.
Values may be sent and summed in bfloat16 or wider, within the bound.
No kernel may reach another device: no remote copies, remote signals or barrier semaphores. Data moves between devices by JAX's collectives and lax.ppermute only.
A program may use at most 64 MiB of HBM per device.

```python
import math
import jax
import jax.numpy as jnp
import numpy as np
from jax import lax

D = 2048
POOL = 1024
FE = 2048
FS = 2048
TOP_K = 4
TOK_B = 128
EXPERTS = 8
CAP = 128
TOKENS_A = 1024
TOKENS_B = 1024
N_EP = 8
N_TP = 4


def spread_rows(key, rows, cols):
    keys = jax.random.split(key, 3)
    row_scale = jnp.exp(jax.random.uniform(keys[0], (rows, 1), jnp.float32, math.log(0.3), math.log(3.0)))
    col_scale = jnp.exp(jax.random.uniform(keys[1], (1, cols), jnp.float32, math.log(0.3), math.log(3.0)))
    base = jax.random.normal(keys[2], (rows, cols), jnp.float32)
    return jnp.clip(base * row_scale * col_scale, -8.0, 8.0).astype(jnp.bfloat16)


def draw_mix_input(key, part):
    return spread_rows(jax.random.fold_in(key, 11), TOKENS_A, D)


def draw_expert_input(key, part):
    return spread_rows(jax.random.fold_in(key, 23), TOKENS_B, D)


def draw_pool_scale(key, part):
    channel = jnp.arange(POOL, dtype=jnp.float32) / POOL
    factor = jnp.exp(jax.random.uniform(jax.random.fold_in(key, 37), (POOL,), jnp.float32, math.log(0.5), math.log(2.0)))
    rising = jnp.exp(math.log(6.0) * channel)
    return 0.5 * rising * factor


def with_spikes(values, own_key, source, target, blocks, factor):
    def block_of(axis_at):
        return (jnp.arange(values.shape[axis_at]) // (values.shape[axis_at] // blocks)).reshape((-1,) + (1,) * (values.ndim - 1 - axis_at))

    near = jax.random.permutation(own_key, blocks)[block_of(target)]
    other_side = (block_of(target) + blocks // 2) % blocks
    return jnp.where((block_of(source) == near) | (block_of(source) == other_side), factor * values, values)


def steps_of(own_key, extent, cuts, low, top_value):
    loudness, own = 1.0, jax.random.fold_in(own_key, 6)
    for axis_at, blocks in cuts:
        steps = jnp.exp(jax.random.uniform(jax.random.fold_in(own, axis_at), (blocks,), jnp.float32, low / len(cuts), top_value / len(cuts)))
        loudness = loudness * jnp.repeat(steps, extent[axis_at] // blocks).reshape([-1 if axis == axis_at else 1 for axis in range(len(extent))])
    return loudness


def routed_block(own_key, own, number, rows, number_of, top, reach, slope):
    order = jax.random.permutation(own_key, number_of)
    heavy_load, usual = load_shares(number_of, rows * top, reach, slope, True), load_shares(number_of, rows * top, reach, slope, False)
    places = jnp.arange(number_of)

    def named(tallies, turn):
        used = int((tallies > 0).sum())
        fixed = max(1, used // 4)
        passed = fixed + (places - fixed + turn * (used - fixed)) % max(1, number_of - fixed)
        return jnp.zeros((number_of,), jnp.int32).at[order[jnp.where(places < fixed, places, passed)]].set(jnp.asarray(tallies, jnp.int32))

    tallies = jnp.where(number % 4 == 0, named(heavy_load, number // 4), named(usual, number - number // 4 - 1))
    mixed = jax.random.permutation(jax.random.fold_in(own, 3), number_of)
    source_of, receiver = mixed[0:number_of // 2 * 2:2], mixed[1:number_of // 2 * 2:2]
    slack = jnp.minimum(tallies[source_of] - 1, reach - tallies[receiver]) // 2
    slack = jnp.where((source_of == order[0]) | (receiver == order[0]) | (tallies[receiver] == 0), 0, jnp.maximum(slack, 0))
    passed = jax.random.randint(jax.random.fold_in(own, 4), (number_of // 2,), 0, 1 << 20) % (slack + 1)
    tallies = tallies.at[source_of].add(-passed).at[receiver].add(passed)
    items = jnp.searchsorted(jnp.cumsum(tallies), jnp.arange(rows * top), side="right").astype(jnp.int32)
    grid = items.reshape(top, rows).T
    grid = grid[jax.random.permutation(jax.random.fold_in(own, 1), rows)]
    turn = jax.random.randint(jax.random.fold_in(own, 2), (rows, 1), 0, top)
    return jnp.take_along_axis(grid, (jnp.arange(top)[None, :] + turn) % top, axis=1)


def load_shares(number_of, total, most, skew, full):
    loads = [(1 << 20) // math.isqrt(grade ** skew) + 1 for grade in range(1, number_of + 1)]
    largest = most if full else min(most, max(-(-total // number_of), total * loads[0] // sum(loads)))
    least = 1 if total - largest >= number_of - 1 else 0
    given, rest = [largest] + [least] * (number_of - 1), total - largest - least * (number_of - 1)
    while rest > 0:
        candidates = [i for i in range(1, number_of) if given[i] < largest] or [i for i in range(1, number_of) if given[i] < most]
        mass, budget = sum([loads[i] for i in candidates]), rest
        for i in candidates:
            more = min(most - given[i], max(1, budget * loads[i] // mass), rest)
            given[i] = given[i] + more
            rest = rest - more
    return np.array(given)


def bell_draw(stream_key, shape, spread, bound, pieces=(), kind=jnp.bfloat16):
    values = spread * jax.random.normal(stream_key, shape, jnp.float32)
    if pieces:
        values = values * steps_of(stream_key, shape, pieces, -0.22, 0.18)
    return jnp.clip(values, -bound, bound).astype(kind)


def gaussian_with(own_key, dims, deviation, reach, pieces, heavy, held_as=jnp.bfloat16):
    values = deviation * jax.random.normal(own_key, dims, jnp.float32)
    if pieces:
        values = values * steps_of(own_key, dims, pieces, -0.22, 0.18)
    return jnp.clip(with_spikes(values, jax.random.fold_in(own_key, 3), *heavy), -reach, reach).astype(held_as)


def setup_inputs(seed: int = 0) -> dict:
    arg_keys = jax.random.split(jax.random.key(seed), 17)
    mix_input = draw_mix_input(jax.random.fold_in(arg_keys[16], 71), 0)
    expert_input = draw_expert_input(jax.random.fold_in(arg_keys[16], 71), 0)
    mix_gain = jnp.clip(1.0 + 0.18 * jax.random.normal(arg_keys[2], (D,), jnp.float32), 0.1, 1.9)
    moe_gain = jnp.clip(1.0 + 0.18 * jax.random.normal(arg_keys[3], (D,), jnp.float32), 0.1, 1.9)
    pool_in = bell_draw(arg_keys[4], (D, POOL), D ** -0.5, 0.125, ((1, 4),))
    pool_scale = draw_pool_scale(jax.random.fold_in(arg_keys[16], 71), 0)
    pool_gain = jnp.clip(1.0 + 0.18 * jax.random.normal(arg_keys[6], (POOL,), jnp.float32), 0.1, 1.9)
    pool_out = bell_draw(arg_keys[7], (POOL, D), POOL ** -0.5, 0.1875, ((1, 4),))
    route_keys = jax.random.split(jax.random.fold_in(arg_keys[8], 1), TOKENS_B // TOK_B)
    route_turns = jax.random.permutation(jax.random.fold_in(arg_keys[8], 3), TOKENS_B // TOK_B)
    route = jax.vmap(lambda own, number: routed_block(jax.random.fold_in(arg_keys[8], 2), own, number, TOK_B, EXPERTS, TOP_K, CAP, 2))(route_keys, route_turns).reshape((TOKENS_B, TOP_K))
    route_score = jnp.clip(0.05 + 0.95 * jax.random.uniform(arg_keys[9], (TOKENS_B, TOP_K), jnp.float32) ** steps_of(arg_keys[9], (TOKENS_B, TOP_K), ((0, 8),), -0.2, 0.2), 0.05, 1.0)
    expert_gate = bell_draw(arg_keys[10], (EXPERTS, D, FE), D ** -0.5, 0.125, ((0, 8), (2, 4)))
    expert_up = bell_draw(arg_keys[11], (EXPERTS, D, FE), D ** -0.5, 0.125, ((0, 8), (2, 4)))
    expert_down = gaussian_with(arg_keys[12], (EXPERTS, FE, D), FE ** -0.5, 0.1875, ((0, 8), (1, 4)), (1, 2, 4, 2.0))
    shared_gate = bell_draw(arg_keys[13], (D, FS), D ** -0.5, 0.125, ((1, 4),))
    shared_up = bell_draw(arg_keys[14], (D, FS), D ** -0.5, 0.125, ((1, 4),))
    shared_down = bell_draw(arg_keys[15], (FS, D), FS ** -0.5, 0.125, ((1, 4),))
    return {"mix_input": mix_input, "expert_input": expert_input, "mix_gain": mix_gain, "moe_gain": moe_gain, "pool_in": pool_in, "pool_scale": pool_scale, "pool_gain": pool_gain, "pool_out": pool_out, "route": route, "route_score": route_score, "expert_gate": expert_gate, "expert_up": expert_up, "expert_down": expert_down, "shared_gate": shared_gate, "shared_up": shared_up, "shared_down": shared_down}


epsilon = 1e-06
reach_rows = 15
window_widths = (2, 4, 8, 16)

def row_norm(rows, gain):
    values = rows.astype(jnp.float32)
    scale = lax.rsqrt(lax.optimization_barrier(jnp.mean(values * values, axis=-1, keepdims=True)) + epsilon)
    return (values * scale * gain.astype(jnp.float32)).astype(jnp.bfloat16)

def window_means(extended, position, group, n_rows):
    total = jnp.zeros((n_rows, extended.shape[1]), jnp.float32)
    result = jnp.zeros((n_rows, extended.shape[1]), jnp.float32)
    for lag in range(16):
        total = total + extended[reach_rows - lag:reach_rows - lag + n_rows]
        for index, width in enumerate(window_widths):
            if lag + 1 == width:
                count = jnp.minimum(position, float(width))[:, None]
                result = jnp.where(group[None, :] == index, total / count, result)
    return result - extended[reach_rows:]

def reference(mix_input, expert_input, mix_gain, moe_gain, pool_in, pool_scale, pool_gain, pool_out, route, route_score, expert_gate, expert_up, expert_down, shared_gate, shared_up, shared_down):
    mix_norm = row_norm(mix_input, mix_gain)
    pool_input = jnp.dot(mix_norm, pool_in, preferred_element_type=jnp.float32).astype(jnp.bfloat16)
    extended = jnp.concatenate([jnp.zeros((reach_rows, POOL), jnp.float32), pool_input.astype(jnp.float32)], axis=0)
    position = jnp.arange(1, TOKENS_A + 1, dtype=jnp.int32).astype(jnp.float32)
    group = jnp.arange(POOL, dtype=jnp.int32) // (POOL // 4)
    scaled = window_means(extended, position, group, TOKENS_A) * pool_scale
    pooled_norm = (scaled * lax.rsqrt(lax.optimization_barrier(jnp.mean(scaled * scaled, axis=1, keepdims=True)) + epsilon) * pool_gain).astype(jnp.bfloat16)
    mix_out = jnp.dot(pooled_norm, pool_out, preferred_element_type=jnp.float32).astype(jnp.bfloat16)
    moe_norm = row_norm(expert_input, moe_gain)
    weights = 2.5 * route_score / lax.optimization_barrier(jnp.sum(route_score, axis=1, keepdims=True))
    most_rows = CAP * N_EP

    def one_expert(routed, expert):
        hit = route == expert
        taken = jnp.any(hit, axis=1)
        order = jnp.argsort(jnp.where(taken, 0, 1).astype(jnp.int32), stable=True)[:most_rows].astype(jnp.int32)
        live = taken[order]
        rows = moe_norm[order]
        gate = jnp.dot(rows, expert_gate[expert], preferred_element_type=jnp.float32)
        upper = jnp.dot(rows, expert_up[expert], preferred_element_type=jnp.float32)
        hidden = (jax.nn.silu(gate) * upper).astype(jnp.bfloat16)
        blocks = hidden.reshape(most_rows, N_TP, FE // N_TP).astype(jnp.float32)
        down = expert_down[expert].reshape(N_TP, FE // N_TP, D).astype(jnp.float32)
        partial_value = jnp.einsum('rpf,pfd->rpd', blocks, down).astype(jnp.bfloat16)
        result = lax.optimization_barrier(jnp.sum(partial_value.astype(jnp.float32), axis=1)).astype(jnp.bfloat16)
        factor = lax.optimization_barrier(jnp.sum(jnp.where(hit, weights, 0.0), axis=1))[order] * live
        routed = routed.at[order].add(result.astype(jnp.float32) * factor[:, None])
        return (routed, None)
    routed, _ = lax.scan(one_expert, jnp.zeros((TOKENS_B, D), jnp.float32), jnp.arange(EXPERTS, dtype=jnp.int32))
    shared_hidden = (jax.nn.silu(jnp.dot(moe_norm, shared_gate, preferred_element_type=jnp.float32)) * jnp.dot(moe_norm, shared_up, preferred_element_type=jnp.float32)).astype(jnp.bfloat16)
    shared = jnp.dot(shared_hidden, shared_down, preferred_element_type=jnp.float32)
    moe_out = (routed + shared).astype(jnp.bfloat16)
    return (mix_out, moe_out)
```

```python
import functools

import jax
import jax.numpy as jnp
from jax import lax
from jax.experimental import pallas as pl
from jax.experimental.pallas import tpu as pltpu
from jax.sharding import PartitionSpec as P

epsilon = 1e-06
reach_rows = 15
window_widths = (2, 4, 8, 16)
CORES = 2
GROUPS = 3
AXES = ("ep", "tp")
VMEM = pl.BlockSpec(memory_space=pltpu.VMEM)


def side_of(size):
    side = 1
    while side * side < size:
        side *= 2
    assert side * side == size
    return side


def routes(n_ep, n_tp, move):
    side = side_of(n_tp)
    pairs = []
    for ep in range(n_ep):
        for tp in range(n_tp):
            z, core, y, x = move(ep // CORES, ep % CORES, tp // side, tp % side)
            pairs.append((ep * n_tp + tp, (z * CORES + core) * n_tp + y * side + x))
    return pairs


def sent(value, n_ep, n_tp, move):
    return lax.ppermute(value, AXES, routes(n_ep, n_tp, move))


def along_z(distance):
    return lambda z, c, y, x: (z ^ distance, c, y, x)


def other_core(z, c, y, x):
    return (z, 1 - c, y, x)


def first_axis(step):
    return lambda z, c, y, x: (z, c, y, x ^ step) if c == 0 else (z, c, y ^ step, x)


def second_axis(step):
    return lambda z, c, y, x: (z, c, y ^ step, x) if c == 0 else (z, c, y, x ^ step)


def column_at(first, second, side):
    core = lax.rem(lax.axis_index("ep"), CORES)
    other = jnp.where(core == 0, second * side + first, first * side + second)
    return lax.bitwise_xor(lax.axis_index("tp"), other.astype(jnp.int32))


def gathered(block, n_ep, n_tp):
    side = side_of(n_tp)
    near = [block] + [sent(block, n_ep, n_tp, first_axis(u)) for u in range(1, side)]
    packed = jnp.concatenate(near, axis=0)
    return near + [sent(packed, n_ep, n_tp, second_axis(u)) for u in range(1, side)]


def silu(value):
    return value / (1.0 + jnp.exp(-value))


def row_norm(rows, gain):
    values = rows.astype(jnp.float32)
    scale = lax.rsqrt(jnp.mean(values * values, axis=-1, keepdims=True) + epsilon)
    return (values * scale * gain).astype(jnp.bfloat16)


def window_means(extended, position, group, n_rows):
    total = jnp.zeros((n_rows, extended.shape[1]), jnp.float32)
    result = jnp.zeros((n_rows, extended.shape[1]), jnp.float32)
    for lag in range(16):
        total = total + extended[reach_rows - lag : reach_rows - lag + n_rows]
        for index, width in enumerate(window_widths):
            if lag + 1 == width:
                count = jnp.minimum(position, float(width))[:, None]
                result = jnp.where(group[None, :] == index, total / count, result)
    return result - extended[reach_rows:]


def norm_kernel(experts, part, x_ref, gain_ref, route_ref, score_ref, all_ref, part_ref):
    width = x_ref.shape[1]

    def rows_of(rows):
        x = x_ref[rows, :].astype(jnp.float32)
        scale = lax.rsqrt(jnp.mean(x * x, axis=1, keepdims=True) + epsilon)
        score = score_ref[rows, :]
        share = 2.5 * score / jnp.sum(score, axis=1, keepdims=True)
        chosen = route_ref[rows, :]
        lanes = lax.broadcasted_iota(jnp.int32, (x.shape[0], all_ref.shape[1] - width), 1)
        expert = jnp.where(lanes < experts, lanes, lanes - experts)
        weight = jnp.zeros(lanes.shape, jnp.float32)
        for k in range(score.shape[1]):
            weight = weight + jnp.where(chosen[:, k : k + 1] == expert, share[:, k : k + 1], 0.0)
        high = weight.astype(jnp.bfloat16)
        low = (weight - high.astype(jnp.float32)).astype(jnp.bfloat16)
        return (x * scale * gain_ref[...]).astype(jnp.bfloat16), jnp.where(
            lanes < experts, high, low
        )

    for target, rows in (
        (part_ref, pl.ds(pl.multiple_of(lax.axis_index("tp") * part, part), part)),
        (all_ref, slice(None)),
    ):
        values, weights = rows_of(rows)
        target[:, :width] = values
        target[:, width:] = weights


def normalized(x, gain, route, score, experts, part):
    lanes = -(-2 * experts // 128) * 128
    shapes = (
        jax.ShapeDtypeStruct((x.shape[0], x.shape[1] + lanes), jnp.bfloat16),
        jax.ShapeDtypeStruct((part, x.shape[1] + lanes), jnp.bfloat16),
    )
    return pl.pallas_call(
        functools.partial(norm_kernel, experts, part),
        out_shape=shapes,
        in_specs=[VMEM] * 4,
        out_specs=(VMEM, VMEM),
        name="row_norm",
    )(x, gain[None, :], route, score)


def expert_kernel(n_pieces, blocks, side, experts, *refs):
    pieces, weights = refs[:n_pieces], refs[n_pieces : n_pieces + 6]
    outs = refs[n_pieces + 6 : n_pieces + 6 + side]
    rows_ref = refs[n_pieces + 6 + side]
    width = weights[0].shape[1]
    n_cols = side * side
    if n_pieces == 1:
        source = pieces[0]
    else:
        source = rows_ref
        part = pieces[0].shape[0] // blocks
        for index, ref in enumerate(pieces):
            for slab in range(ref.shape[0] // (part * blocks)):
                first, second = (index, 0) if index < side else (slab, index - side + 1)
                place = column_at(first, second, side) * part
                for block in range(blocks):
                    start = pl.multiple_of(place + block * part * n_cols, part)
                    at = (slab * blocks + block) * part
                    rows_ref[pl.ds(start, part), :] = ref[at : at + part, :]
    x = source[:, :width]
    extra = source[:, width:].astype(jnp.float32)
    lanes = lax.broadcasted_iota(jnp.int32, extra.shape, 1)
    ep = lax.axis_index("ep")
    hidden = []
    local = weights[0].shape[0]
    for half in range(2):
        gate_ref, up_ref, _ = weights[3 * half : 3 * half + 3]
        owner = ep if half == 0 else lax.bitwise_xor(ep, 1)
        for one in range(local):
            name = owner * local + one
            mine = (lanes == name) | (lanes == name + experts)
            weight = jnp.sum(jnp.where(mine, extra, 0.0), axis=1, keepdims=True)
            gate = jnp.dot(x, gate_ref[one], preferred_element_type=jnp.float32)
            upper = jnp.dot(x, up_ref[one], preferred_element_type=jnp.float32)
            hidden.append((silu(gate) * upper * weight).astype(jnp.bfloat16))
    span = weights[2].shape[2] // n_cols
    for first in range(side):
        for second in range(side):
            start = pl.multiple_of(column_at(first, second, side) * span, span)
            total = jnp.zeros((x.shape[0], span), jnp.float32)
            for half in range(2):
                down_ref = weights[3 * half + 2]
                for one in range(local):
                    total = total + jnp.dot(
                        hidden[half * local + one],
                        down_ref[one, :, pl.ds(start, span)],
                        preferred_element_type=jnp.float32,
                    )
            at = second * span
            outs[first][:, at : at + span] = total.astype(outs[first].dtype)


def expert_partials(pieces, weights, blocks, side, experts, index):
    rows = sum(piece.shape[0] for piece in pieces)
    width = weights[2].shape[2] // side
    shapes = [
        jax.ShapeDtypeStruct((rows, width), jnp.float32 if u == 0 else jnp.bfloat16)
        for u in range(side)
    ]
    whole_rows = 16 if len(pieces) == 1 else rows
    return pl.pallas_call(
        functools.partial(expert_kernel, len(pieces), blocks, side, experts),
        out_shape=shapes,
        in_specs=[VMEM] * (len(pieces) + 6),
        out_specs=[VMEM] * side,
        scratch_shapes=[pltpu.VMEM((whole_rows, pieces[0].shape[1]), jnp.bfloat16)],
        name=f"experts_{index}",
        compiler_params=pltpu.CompilerParams(vmem_limit_bytes=40 << 20),
    )(*pieces, *weights)


def outputs_kernel(side, shared_width, channels, pool_width, *refs):
    n_pieces = 2 * side - 1
    pieces = refs[:n_pieces]
    down_ref, pool_ref, mix_ref, shared_ref = refs[n_pieces:]
    rows = mix_ref.shape[0]
    mix = jnp.zeros(mix_ref.shape, jnp.float32)
    shared = jnp.zeros(shared_ref.shape, jnp.float32)
    squares = jnp.zeros((rows, 1), jnp.float32)
    tail = shared_width + -(-channels // 128) * 128
    for index, ref in enumerate(pieces):
        for slab in range(ref.shape[0] // rows):
            first, second = (index, 0) if index < side else (slab, index - side + 1)
            column = column_at(first, second, side)
            block = slice(slab * rows, (slab + 1) * rows)
            at = pl.ds(pl.multiple_of(column * shared_width, shared_width), shared_width)
            shared = shared + jnp.dot(
                ref[block, :shared_width], down_ref[at, :], preferred_element_type=jnp.float32
            )
            at = pl.ds(pl.multiple_of(column * channels, channels), channels)
            mix = mix + jnp.dot(
                ref[block, shared_width : shared_width + channels],
                pool_ref[at, :],
                preferred_element_type=jnp.float32,
            )
            squares = squares + jnp.sum(
                ref[block, tail:].astype(jnp.float32), axis=1, keepdims=True
            )
    scale = lax.rsqrt(squares / pool_width + epsilon)
    mix_ref[...] = (mix * scale).astype(mix_ref.dtype)
    shared_ref[...] = shared


def outputs(pieces, shared_down, pool_out, side, shared_width, channels):
    rows, span = pieces[0].shape[0], pool_out.shape[1]
    return pl.pallas_call(
        functools.partial(outputs_kernel, side, shared_width, channels, pool_out.shape[0]),
        out_shape=(
            jax.ShapeDtypeStruct((rows, span), jnp.bfloat16),
            jax.ShapeDtypeStruct((rows, span), jnp.float32),
        ),
        in_specs=[VMEM] * (len(pieces) + 2),
        out_specs=(VMEM, VMEM),
        name="outputs",
    )(*pieces, shared_down, pool_out)


def on_device(
    mix_input,
    expert_input,
    mix_gain,
    moe_gain,
    pool_in,
    pool_scale,
    pool_gain,
    pool_out,
    route,
    route_score,
    expert_gate,
    expert_up,
    expert_down,
    shared_gate,
    shared_up,
    shared_down,
):
    n_ep, n_tp = lax.axis_size("ep"), lax.axis_size("tp")
    side, n_z = side_of(n_tp), n_ep // CORES
    tok_rows, channels = mix_input.shape[0], pool_in.shape[1]
    experts = expert_gate.shape[0] * n_ep
    width = pool_out.shape[1]
    send = functools.partial(sent, n_ep=n_ep, n_tp=n_tp)

    all_rows, part_rows = normalized(
        expert_input, moe_gain, route, route_score, experts, tok_rows // n_tp
    )
    from_z = {d: send(part_rows, move=along_z(d)) for d in range(1, n_z)}
    own = (expert_gate, expert_up, expert_down)
    weights = own + tuple(send(w, move=other_core) for w in own)

    mix_norm = row_norm(mix_input, mix_gain)
    pool_input = jnp.dot(mix_norm, pool_in, preferred_element_type=jnp.float32).astype(jnp.bfloat16)
    ahead = [(i * n_tp + j, (i + 1) * n_tp + j) for i in range(n_ep - 1) for j in range(n_tp)]
    before = lax.ppermute(pool_input[tok_rows - reach_rows :], AXES, ahead)
    extended = jnp.concatenate([before, pool_input], axis=0).astype(jnp.float32)
    position = (lax.axis_index("ep") * tok_rows + jnp.arange(tok_rows, dtype=jnp.int32) + 1).astype(
        jnp.float32
    )
    channel_ids = lax.axis_index("tp") * channels + jnp.arange(channels, dtype=jnp.int32)
    group = channel_ids // (channels * n_tp // 4)
    scaled = window_means(extended, position, group, tok_rows) * pool_scale
    squares = jnp.sum(scaled * scaled, axis=1, keepdims=True)
    high = squares.astype(jnp.bfloat16)
    low = (squares - high.astype(jnp.float32)).astype(jnp.bfloat16)
    model_width = expert_input.shape[1]
    shared_hidden = (
        silu(jnp.dot(all_rows[:, :model_width], shared_gate, preferred_element_type=jnp.float32))
        * jnp.dot(all_rows[:, :model_width], shared_up, preferred_element_type=jnp.float32)
    ).astype(jnp.bfloat16)
    filler = -channels % 128
    payload = jnp.concatenate(
        [
            shared_hidden,
            jnp.pad((scaled * pool_gain).astype(jnp.bfloat16), ((0, 0), (0, filler))),
            jnp.pad(jnp.concatenate([high, low], axis=1), ((0, 0), (0, 126))),
        ],
        axis=1,
    )
    pieces = gathered(payload, n_ep, n_tp)
    mix_out, shared_part = outputs(
        pieces, shared_down, pool_out, side, shared_hidden.shape[1], channels
    )

    far = list(range(1, n_z))
    per = -(-len(far) // GROUPS)
    plans = [[0]] + [far[i : i + per] for i in range(0, len(far), per)]
    moe = shared_part
    for index, plan in enumerate(plans):
        if index == 0:
            blocks = [all_rows]
        else:
            mine = jnp.concatenate([from_z[d] for d in plan], axis=0)
            blocks = gathered(mine, n_ep, n_tp)
        outs = expert_partials(blocks, weights, len(plan), side, experts, index)
        total = outs[0]
        for u in range(1, side):
            total = total + send(outs[u], move=first_axis(u)).astype(jnp.float32)
        result = total[:, :width]
        for u in range(1, side):
            piece = total[:, u * width : (u + 1) * width].astype(jnp.bfloat16)
            result = result + send(piece, move=second_axis(u)).astype(jnp.float32)
        if index == 0:
            moe = moe + result
        else:
            result = result.astype(jnp.bfloat16)
            for place, d in enumerate(plan):
                block = result[place * tok_rows : (place + 1) * tok_rows]
                moe = moe + send(block, move=along_z(d)).astype(jnp.float32)
    return (mix_out, moe.astype(jnp.bfloat16))


def solution(mesh):
    return jax.shard_map(
        on_device,
        mesh=mesh,
        in_specs=(
            P("ep", None),
            P("ep", None),
            P(),
            P(),
            P(None, "tp"),
            P("tp"),
            P("tp"),
            P(None, "tp"),
            P("ep", None),
            P("ep", None),
            P("ep", None, "tp"),
            P("ep", None, "tp"),
            P("ep", "tp", None),
            P(None, "tp"),
            P(None, "tp"),
            P(None, "tp"),
        ),
        out_specs=(P("ep", "tp"), P("ep", "tp")),
        check_vma=False,
    )
```
